32 devices in a mesh: sp: 8 (over z, y), dp: 4 (over x, core).
Axes of the slice: x: 2, y: 2, z: 4, core: 2. Of those that a mesh axis runs over, the one named last changes fastest.
Arguments:
- out_cotangent: bfloat16 [4, 2048, 2048], P('dp', 'sp'), may hold values from -6 to 6
- value_pre: bfloat16 [4, 2048, 2048], P('dp', 'sp'), may hold values from -8 to 8
- gate_pre: bfloat16 [4, 2048, 2048], P('dp', 'sp'), may hold values from -8 to 8
- out_weight: bfloat16 [2048, 2048], P('dp'), may hold values from -0.125 to 0.125
- conv_kernel: bfloat16 [31, 2048], P(None, 'sp'), may hold values from -6 to 6
- norm_gain: bfloat16 [2048], P('sp'), may hold values from 0.099609375 to 1.8984375
Outputs:
- grad_value: bfloat16 [4, 2048, 2048], P('dp', 'sp')
- grad_gate: bfloat16 [4, 2048, 2048], P('dp', 'sp')
- grad_out_weight: float32 [2048, 2048], P(('sp', 'dp'))
- grad_kernel: float32 [31, 2048], P(None, 'sp')
- grad_gain: float32 [2048], P('sp')
The draws below stay inside these ranges and needn't reach their ends.
All inputs are finite; a program needn't handle non-finite values.
Results may differ from the reference program's by a relative error of at most 0.011.
Values may be sent and summed in bfloat16 or wider, within the bound.
No kernel may reach another device: no remote copies, remote signals or barrier semaphores. Data moves between devices by JAX's collectives and lax.ppermute only.
A program may use at most 128 MiB of HBM per device.

```python
import math
import jax
import jax.numpy as jnp
from jax import lax

D = 2048
CONV_W = 31
SEQS = 4
LENGTH = 2048
TOKENS = 8192


def draw_value_pre(key, part):
    keys = jax.random.split(jax.random.fold_in(key, 11), 2)
    shape = (SEQS, LENGTH, D)
    row_scale = jnp.exp(jax.random.uniform(keys[1], (SEQS, LENGTH, 1), jnp.float32, math.log(0.4), math.log(2.5)))
    values_out = jax.random.normal(keys[0], shape, jnp.float32) * row_scale
    return jnp.clip(values_out, -8.0, 8.0).astype(jnp.bfloat16)


def draw_conv_kernel(key, part):
    keys = jax.random.split(jax.random.fold_in(key, 23), 2)
    position = jnp.arange(D, dtype=jnp.float32) / float(D)
    rough = jnp.exp(jax.random.uniform(keys[1], (1, D), jnp.float32, math.log(0.5), math.log(2.0)))
    column_scale = jnp.exp(math.log(6.0) * position)[None, :] * rough
    taps = jax.random.normal(keys[0], (CONV_W, D), jnp.float32)
    taps = taps * column_scale * float(CONV_W) ** (-0.5)
    return jnp.clip(taps, -6.0, 6.0).astype(jnp.bfloat16)


def shard_levels(rng, shape, pieces, low, high):
    def one(axis_at, blocks):
        steps = jax.random.uniform(jax.random.fold_in(jax.random.fold_in(rng, 6), axis_at), (blocks,), jnp.float32, low / len(pieces), high / len(pieces))
        return jnp.repeat(jnp.exp(steps), shape[axis_at] // blocks).reshape((-1,) + (1,) * (len(shape) - axis_at - 1))

    gain = one(*pieces[0])
    for cut in pieces[1:]:
        gain = gain * one(*cut)
    return gain


def normal_values(rng, shape, spread, limit, cuts=(), kind=jnp.bfloat16):
    values = jax.random.normal(rng, shape, jnp.float32) * spread
    if len(cuts) > 0:
        values = shard_levels(rng, shape, cuts, -0.22, 0.18) * values
    return jnp.clip(values, min=-limit, max=limit).astype(kind)


def setup_inputs(seed: int = 0) -> dict:
    key_list = jax.random.split(jax.random.key(seed), 7)
    out_cotangent = normal_values(key_list[0], (SEQS, LENGTH, D), 1.0, 6.0, ((0, 4), (1, 8)))
    value_pre = draw_value_pre(jax.random.fold_in(key_list[6], 71), 0)
    gate_pre = normal_values(key_list[2], (SEQS, LENGTH, D), 1.5, 8.0, ((0, 4), (1, 8)))
    out_weight = normal_values(key_list[3], (D, D), D ** -0.5, 0.125, ((0, 4),))
    conv_kernel = draw_conv_kernel(jax.random.fold_in(key_list[6], 71), 0)
    norm_gain = jnp.clip(1.0 + 0.18 * jax.random.normal(key_list[5], (D,), jnp.float32), 0.099609375, 1.8984375).astype(jnp.bfloat16)
    return {"out_cotangent": out_cotangent, "value_pre": value_pre, "gate_pre": gate_pre, "out_weight": out_weight, "conv_kernel": conv_kernel, "norm_gain": norm_gain}


epsilon = 1e-05

def shift_down(array, offset):
    return jnp.pad(array, ((offset, 0), (0, 0)))[:array.shape[0]]

def shift_up(array, offset):
    return jnp.pad(array, ((0, offset), (0, 0)))[offset:]

def reference(out_cotangent, value_pre, gate_pre, out_weight, conv_kernel, norm_gain):
    taps_float = conv_kernel.astype(jnp.float32)
    gain_float = norm_gain.astype(jnp.float32)
    weight_sum = jnp.zeros((D, D), jnp.float32)
    kernel_sum = jnp.zeros((CONV_W, D), jnp.float32)
    gain_sum = jnp.zeros((D,), jnp.float32)
    value_grads = []
    gate_grads = []
    for sequence in range(SEQS):
        cotangent = out_cotangent[sequence]
        values_in = value_pre[sequence].astype(jnp.float32)
        sigmoid_gate = jax.nn.sigmoid(gate_pre[sequence].astype(jnp.float32))
        gated = (values_in * sigmoid_gate).astype(jnp.bfloat16)
        gated_float = gated.astype(jnp.float32)
        conv = jnp.zeros(gated_float.shape, jnp.float32)
        for offset in range(CONV_W):
            conv = conv + taps_float[offset] * shift_down(gated_float, offset)
        centre = lax.optimization_barrier(jnp.mean(conv, axis=1, keepdims=True))
        deviation = conv - centre
        variance = lax.optimization_barrier(jnp.mean(deviation * deviation, axis=1, keepdims=True))
        inv_scale = lax.rsqrt(variance + epsilon)
        centred = deviation * inv_scale
        normed = centred * gain_float
        activation = jax.nn.silu(normed).astype(jnp.bfloat16)
        grad_act = lax.dot_general(cotangent, out_weight, (((1,), (1,)), ((), ())), preferred_element_type=jnp.float32).astype(jnp.bfloat16)
        weight_sum = weight_sum + lax.dot_general(activation, cotangent, (((0,), (0,)), ((), ())), preferred_element_type=jnp.float32)
        sig_norm = jax.nn.sigmoid(normed)
        grad_normed = grad_act.astype(jnp.float32) * sig_norm * (1.0 + normed * (1.0 - sig_norm))
        gain_sum = gain_sum + lax.optimization_barrier(jnp.sum(grad_normed * centred, axis=0))
        grad_centred = grad_normed * gain_float
        grad_conv = (grad_centred - lax.optimization_barrier(jnp.mean(grad_centred, axis=1, keepdims=True)) - centred * lax.optimization_barrier(jnp.mean(grad_centred * centred, axis=1, keepdims=True))) * inv_scale
        kernel_rows = [lax.optimization_barrier(jnp.sum(grad_conv * shift_down(gated_float, offset), axis=0)) for offset in range(CONV_W)]
        kernel_sum = kernel_sum + jnp.stack(kernel_rows, axis=0)
        grad_gated = jnp.zeros(grad_conv.shape, jnp.float32)
        for offset in range(CONV_W):
            grad_gated = grad_gated + taps_float[offset] * shift_up(grad_conv, offset)
        grad_gated = grad_gated.astype(jnp.bfloat16).astype(jnp.float32)
        value_grads.append((grad_gated * sigmoid_gate).astype(jnp.bfloat16))
        gate_grads.append((grad_gated * values_in * sigmoid_gate * (1.0 - sigmoid_gate)).astype(jnp.bfloat16))
    factor = float(TOKENS) ** (-0.5)
    return (jnp.stack(value_grads, axis=0), jnp.stack(gate_grads, axis=0), weight_sum * factor, kernel_sum * factor, gain_sum * factor)
```

```python
import jax
import jax.numpy as jnp
from jax import lax
from jax.sharding import PartitionSpec as P

epsilon = 1e-05
CORES = 2


def chip_shift(value, chips, cores, steps):
    pairs = [
        (chip * cores + core, (chip + steps) % chips * cores + core)
        for chip in range(chips)
        for core in range(cores)
    ]
    return lax.ppermute(value, "dp", pairs)


def core_swap(value, chips, cores):
    return lax.ppermute(value, "dp", [(i, i ^ 1) for i in range(chips * cores)])


def bit_swap(value, axis, bit):
    count = lax.axis_size(axis)
    return lax.ppermute(value, axis, [(i, i ^ (1 << bit)) for i in range(count)])


def passed_along(value, axis, steps):
    count = lax.axis_size(axis)
    initial, last = (max(0, -steps), min(count, count - steps))
    return lax.ppermute(value, axis, [(source, source + steps) for source in range(initial, last)])


def gathered(value, axis):
    count = lax.axis_size(axis)
    bits = count.bit_length() - 1
    me = lax.axis_index(axis)
    whole = value[None]
    for bit in range(bits):
        other = bit_swap(whole, axis, bit)
        mine_first = ((me >> bit) & 1) == 0
        whole = jnp.where(
            mine_first,
            jnp.concatenate([whole, other], axis=0),
            jnp.concatenate([other, whole], axis=0),
        )
    return whole.transpose(1, 0, 2).reshape(value.shape[0], -1)


def gated_forward(values_in, gates_in):
    return (values_in.astype(jnp.float32) * jax.nn.sigmoid(gates_in.astype(jnp.float32))).astype(
        jnp.bfloat16
    )


def gated_backward(grad_gated, values_in, gates_in):
    sigmoid_gate = jax.nn.sigmoid(gates_in.astype(jnp.float32))
    grad_float = grad_gated.astype(jnp.float32)
    grad_values = (grad_float * sigmoid_gate).astype(jnp.bfloat16)
    grad_gates = (
        grad_float * values_in.astype(jnp.float32) * sigmoid_gate * (1.0 - sigmoid_gate)
    ).astype(jnp.bfloat16)
    return (grad_values, grad_gates)


def scattered_sum(parts, axis):
    count = lax.axis_size(axis)
    bits = count.bit_length() - 1
    me = lax.axis_index(axis)
    for bit in range(bits):
        mine = (me >> bit) & 1
        pairs = parts.reshape((parts.shape[0] // 2, 2) + parts.shape[1:])
        keep = lax.dynamic_index_in_dim(pairs, mine, axis=1, keepdims=False)
        send = lax.dynamic_index_in_dim(pairs, 1 - mine, axis=1, keepdims=False)
        parts = keep + bit_swap(send.astype(jnp.bfloat16), axis, bit).astype(jnp.float32)
    return parts[0]


def shards(out_cotangent, value_pre, gate_pre, out_weight, conv_kernel, norm_gain):
    cotangent = out_cotangent[0]
    values_in = value_pre[0]
    gates_in = gate_pre[0]
    row_count, width = cotangent.shape
    taps_count = conv_kernel.shape[0]
    margin = taps_count - 1
    sp_count, dp_count = lax.axis_size("sp"), lax.axis_size("dp")
    cores = CORES if dp_count % CORES == 0 else 1
    chips = dp_count // cores
    place = lax.axis_index("dp")
    chip, core = place // cores, place % cores
    width_float = float(width)

    small = gathered(jnp.concatenate([conv_kernel, norm_gain[None]], axis=0), "sp")
    front_rows = passed_along(
        gated_forward(values_in[row_count - margin :], gates_in[row_count - margin :]), "sp", 1
    )
    cots = [cotangent] + [chip_shift(cotangent, chips, cores, k) for k in range(1, chips)]
    weight_other = core_swap(out_weight, chips, cores)

    def times_weights(cot):
        dims = (((1,), (1,)), ((), ()))
        mine = lax.dot_general(cot, out_weight, dims, preferred_element_type=jnp.float32)
        other = lax.dot_general(cot, weight_other, dims, preferred_element_type=jnp.float32)
        mine, other = mine.astype(jnp.bfloat16), other.astype(jnp.bfloat16)
        return jnp.where(
            core == 0,
            jnp.concatenate([mine, other], axis=1),
            jnp.concatenate([other, mine], axis=1),
        )

    grad_act = jnp.zeros((row_count, width), jnp.bfloat16)
    for k in range(chips):
        piece = times_weights(cots[k])
        if k:
            piece = chip_shift(piece, chips, cores, -k)
        grad_act = lax.dynamic_update_slice(
            grad_act, piece, (0, (chip + k) % chips * piece.shape[1])
        )

    taps_float = small[:taps_count].astype(jnp.float32)
    gain_float = small[taps_count].astype(jnp.float32)
    gated = gated_forward(values_in, gates_in)
    extended = jnp.concatenate([front_rows, gated], axis=0).astype(jnp.float32)
    conv = jnp.zeros((row_count, width), jnp.float32)
    for offset in range(taps_count):
        begin = margin - offset
        conv = conv + taps_float[offset] * extended[begin : begin + row_count]
    centre = (jnp.sum(conv, axis=1) / width_float)[:, None]
    variance = (jnp.sum(conv * conv, axis=1) / width_float)[:, None] - centre * centre
    inv_scale = lax.rsqrt(variance + epsilon)
    centred = (conv - centre) * inv_scale
    normed = centred * gain_float
    sig_norm = jax.nn.sigmoid(normed)
    activation = (normed * sig_norm).astype(jnp.bfloat16)

    rows_out = width // (sp_count * dp_count)
    act_rows = activation.T.reshape(sp_count, chips, cores, rows_out, row_count)

    def for_chip(k):
        return lax.dynamic_index_in_dim(act_rows, (chip + k) % chips, axis=1, keepdims=False)

    acts = [for_chip(0)] + [
        chip_shift(for_chip(k), chips, cores, k) for k in range(1, chips)
    ]
    lefts, rights = [], []
    for act, cot in zip(acts, cots):
        lefts.append(lax.dynamic_index_in_dim(act, core, axis=1, keepdims=False))
        rights.append(cot)
        if cores > 1:
            others = lax.dynamic_index_in_dim(act, 1 - core, axis=1, keepdims=False)
            lefts.append(core_swap(others, chips, cores))
            rights.append(core_swap(cot, chips, cores))
    left = jnp.concatenate(lefts, axis=2).reshape(sp_count * rows_out, -1)
    right = jnp.concatenate(rights, axis=0)
    weight_part = lax.dot_general(
        left, right, (((1,), (0,)), ((), ())), preferred_element_type=jnp.float32
    )
    weight_sum = scattered_sum(weight_part.reshape(sp_count, rows_out, width), "sp")

    grad_normed = grad_act.astype(jnp.float32) * sig_norm * (1.0 + normed * (1.0 - sig_norm))
    gain_part = jnp.sum(grad_normed * centred, axis=0)
    grad_centred = grad_normed * gain_float
    first = jnp.sum(grad_centred, axis=1)
    second = jnp.sum(grad_centred * centred, axis=1)
    grad_conv = (
        grad_centred
        - (first / width_float)[:, None]
        - centred * (second / width_float)[:, None]
    ) * inv_scale
    kernel_rows = []
    for offset in range(taps_count):
        begin = margin - offset
        kernel_rows.append(jnp.sum(grad_conv * extended[begin : begin + row_count], axis=0))
    small_part = jnp.stack(kernel_rows + [gain_part], axis=0)
    small_part = lax.all_to_all(small_part, "sp", 1, 0, tiled=True)
    small_part = jnp.sum(small_part.reshape(sp_count, taps_count + 1, -1), axis=0)
    small_sum = jnp.sum(lax.all_gather(small_part, "dp"), axis=0)

    grad_extended = jnp.concatenate([grad_conv, passed_along(grad_conv[:margin], "sp", -1)], axis=0)
    grad_gated = jnp.zeros(grad_conv.shape, jnp.float32)
    for offset in range(taps_count):
        grad_gated = grad_gated + taps_float[offset] * grad_extended[offset : offset + row_count]
    grad_values, grad_gates = gated_backward(grad_gated.astype(jnp.bfloat16), values_in, gates_in)

    factor = float(sp_count * dp_count * row_count) ** (-0.5)
    return (
        grad_values[None],
        grad_gates[None],
        weight_sum * factor,
        small_sum[:taps_count] * factor,
        small_sum[taps_count] * factor,
    )


def solution(mesh):
    placed = (
        P("dp", "sp", None),
        P("dp", "sp", None),
        P("dp", "sp", None),
        P("dp", None),
        P(None, "sp"),
        P("sp"),
    )
    return jax.shard_map(
        shards,
        mesh=mesh,
        in_specs=placed,
        out_specs=(
            P("dp", "sp", None),
            P("dp", "sp", None),
            P(("sp", "dp"), None),
            P(None, "sp"),
            P("sp"),
        ),
        check_vma=False,
    )
```

```python
import functools

import jax
import jax.numpy as jnp
from jax import lax
from jax.experimental import pallas as pl
from jax.experimental.pallas import tpu as pltpu
from jax.sharding import PartitionSpec as P

epsilon = 1e-05
CORES = 2
LANES = 128
PAD = 32


def sigmoid(value):
    return 1.0 / (1.0 + jnp.exp(-value))


def forward_body(taps_count, value, gate, front, taps, act, centred, gated, inv, held, conv):
    rows, width = value.shape
    columns = width // LANES
    step = pl.program_id(0)

    @pl.when(step == 0)
    def _():
        for c in range(columns):
            held[c, :PAD, :] = front[:, c * LANES : (c + 1) * LANES].astype(jnp.float32)

    @pl.when(step > 0)
    def _():
        for c in range(columns):
            held[c, :PAD, :] = held[c, rows : rows + PAD, :]

    def convolve(c, total):
        lanes = pl.ds(pl.multiple_of(c * LANES, LANES), LANES)
        product = value[:, lanes].astype(jnp.float32) * sigmoid(gate[:, lanes].astype(jnp.float32))
        product = product.astype(jnp.bfloat16)
        gated[:, lanes] = product
        held[c, PAD : PAD + rows, :] = product.astype(jnp.float32)
        result = jnp.zeros((rows, LANES), jnp.float32)
        for k in range(taps_count):
            result = result + taps[c, k : k + 1, :] * held[c, PAD - k : PAD - k + rows, :]
        conv[c] = result
        return total + result

    zeros = jnp.zeros((rows, LANES), jnp.float32)
    total = lax.fori_loop(0, columns, convolve, zeros)
    centre = jnp.sum(total, axis=1, keepdims=True) * (1.0 / width)

    def squares(c, total):
        off = conv[c] - centre
        conv[c] = off
        return total + off * off

    total = lax.fori_loop(0, columns, squares, zeros)
    variance = jnp.sum(total, axis=1, keepdims=True) * (1.0 / width)
    scale = lax.rsqrt(variance + epsilon)
    inv[...] = jnp.broadcast_to(scale, inv.shape)

    def normalize(c, carry):
        lanes = pl.ds(pl.multiple_of(c * LANES, LANES), LANES)
        value_c = conv[c] * scale
        centred[c] = value_c
        normed = value_c * taps[c, taps_count : taps_count + 1, :]
        act[:, lanes] = (normed * sigmoid(normed)).astype(jnp.bfloat16)
        return carry

    lax.fori_loop(0, columns, normalize, 0)


def forward(values_in, gates_in, front, taps, taps_count):
    rows, width = values_in.shape
    columns = width // LANES
    block = 64
    by_rows = pl.BlockSpec((block, width), lambda i: (i, 0))
    return pl.pallas_call(
        functools.partial(forward_body, taps_count),
        grid=(rows // block,),
        in_specs=[
            by_rows,
            by_rows,
            pl.BlockSpec((PAD, width), lambda i: (0, 0)),
            pl.BlockSpec(taps.shape, lambda i: (0, 0, 0)),
        ],
        out_specs=[
            by_rows,
            pl.BlockSpec((columns, block, LANES), lambda i: (0, i, 0)),
            by_rows,
            pl.BlockSpec((block, LANES), lambda i: (i, 0)),
        ],
        out_shape=[
            jax.ShapeDtypeStruct((rows, width), jnp.bfloat16),
            jax.ShapeDtypeStruct((columns, rows, LANES), jnp.float32),
            jax.ShapeDtypeStruct((rows, width), jnp.bfloat16),
            jax.ShapeDtypeStruct((rows, LANES), jnp.float32),
        ],
        scratch_shapes=[
            pltpu.VMEM((columns, PAD + block, LANES), jnp.float32),
            pltpu.VMEM((columns, block, LANES), jnp.float32),
        ],
        cost_estimate=pl.CostEstimate(
            flops=rows * width * 100, bytes_accessed=rows * width * 12, transcendentals=0
        ),
        name="forward",
    )(values_in, gates_in, front, taps)


def normed_back_body(taps_count, grad_act, centred, inv, taps, grad_conv, gain_part, held):
    rows, width = grad_act.shape
    columns = width // LANES

    @pl.when(pl.program_id(0) == 0)
    def _():
        gain_part[...] = jnp.zeros(gain_part.shape, jnp.float32)

    def products(c, totals):
        lanes = pl.ds(pl.multiple_of(c * LANES, LANES), LANES)
        gain = taps[c, taps_count : taps_count + 1, :]
        centred_c = centred[c]
        normed = centred_c * gain
        sig = sigmoid(normed)
        grad_normed = grad_act[:, lanes].astype(jnp.float32) * sig * (1.0 + normed * (1.0 - sig))
        part = (grad_normed * centred_c).reshape(rows // 8, 8, LANES)
        gain_part[:, lanes] += jnp.sum(part, axis=0)
        grad_centred = grad_normed * gain
        held[c] = grad_centred
        return (totals[0] + grad_centred, totals[1] + grad_centred * centred_c)

    zeros = jnp.zeros((rows, LANES), jnp.float32)
    first, second = lax.fori_loop(0, columns, products, (zeros, zeros))
    first = jnp.sum(first, axis=1, keepdims=True) * (1.0 / width)
    second = jnp.sum(second, axis=1, keepdims=True) * (1.0 / width)
    scale = inv[...]

    def finish(c, carry):
        grad_conv[c] = (held[c] - first - centred[c] * second) * scale
        return carry

    lax.fori_loop(0, columns, finish, 0)


def normed_back(grad_act, centred, inv, taps, taps_count):
    rows, width = grad_act.shape
    columns = width // LANES
    block = 64
    by_columns = pl.BlockSpec((columns, block, LANES), lambda i: (0, i, 0))
    return pl.pallas_call(
        functools.partial(normed_back_body, taps_count),
        grid=(rows // block,),
        in_specs=[
            pl.BlockSpec((block, width), lambda i: (i, 0)),
            by_columns,
            pl.BlockSpec((block, LANES), lambda i: (i, 0)),
            pl.BlockSpec(taps.shape, lambda i: (0, 0, 0)),
        ],
        out_specs=[by_columns, pl.BlockSpec((8, width), lambda i: (0, 0))],
        out_shape=[
            jax.ShapeDtypeStruct((columns, rows, LANES), jnp.float32),
            jax.ShapeDtypeStruct((8, width), jnp.float32),
        ],
        scratch_shapes=[pltpu.VMEM((columns, block, LANES), jnp.float32)],
        cost_estimate=pl.CostEstimate(
            flops=rows * width * 40, bytes_accessed=rows * width * 10, transcendentals=0
        ),
        name="normed_back",
    )(grad_act, centred, inv, taps)


def taps_back_body(taps_count, grad_conv, gated, front, gain_part, out, held):
    rows = gated.shape[0]
    held[:PAD, :] = front[...].astype(jnp.float32)
    held[PAD:, :] = gated[...].astype(jnp.float32)
    sums = [jnp.zeros((8, LANES), jnp.float32) for _ in range(taps_count)]
    for j in range(0, rows, 8):
        grad = grad_conv[0, j : j + 8, :]
        for k in range(taps_count):
            begin = j + PAD - k
            sums[k] = sums[k] + grad * held[begin : begin + 8, :]
    for k in range(taps_count):
        out[k : k + 1, :] = jnp.sum(sums[k], axis=0, keepdims=True)
    out[taps_count : taps_count + 1, :] = jnp.sum(gain_part[...], axis=0, keepdims=True)


def taps_back(grad_conv, gated, front, gain_part, taps_count):
    columns, rows, _ = grad_conv.shape
    width = columns * LANES
    return pl.pallas_call(
        functools.partial(taps_back_body, taps_count),
        grid=(columns,),
        in_specs=[
            pl.BlockSpec((1, rows, LANES), lambda c: (c, 0, 0)),
            pl.BlockSpec((rows, LANES), lambda c: (0, c)),
            pl.BlockSpec((PAD, LANES), lambda c: (0, c)),
            pl.BlockSpec((8, LANES), lambda c: (0, c)),
        ],
        out_specs=pl.BlockSpec((taps_count + 1, LANES), lambda c: (0, c)),
        out_shape=jax.ShapeDtypeStruct((taps_count + 1, width), jnp.float32),
        scratch_shapes=[pltpu.VMEM((PAD + rows, LANES), jnp.float32)],
        cost_estimate=pl.CostEstimate(
            flops=rows * width * 62, bytes_accessed=rows * width * 6, transcendentals=0
        ),
        name="taps_back",
    )(grad_conv, gated, front, gain_part)


def gated_back_body(taps_count, grad_conv, after, taps, value, gate, grad_value, grad_gate, held):
    rows = value.shape[0]
    block = 64
    held[:rows, :] = grad_conv[0]
    held[rows:, :] = after[0]
    for begin in range(0, rows, block):
        result = jnp.zeros((block, LANES), jnp.float32)
        for k in range(taps_count):
            result = result + taps[0, k : k + 1, :] * held[begin + k : begin + k + block, :]
        result = result.astype(jnp.bfloat16).astype(jnp.float32)
        sig = sigmoid(gate[begin : begin + block, :].astype(jnp.float32))
        grad_sig = result * sig
        grad_value[begin : begin + block, :] = grad_sig.astype(jnp.bfloat16)
        grad_gate[begin : begin + block, :] = (
            grad_sig * value[begin : begin + block, :].astype(jnp.float32) * (1.0 - sig)
        ).astype(jnp.bfloat16)


def gated_back(grad_conv, after, taps, values_in, gates_in, taps_count):
    columns, rows, _ = grad_conv.shape
    width = columns * LANES
    flat = pl.BlockSpec((rows, LANES), lambda c: (0, c))
    return pl.pallas_call(
        functools.partial(gated_back_body, taps_count),
        grid=(columns,),
        in_specs=[
            pl.BlockSpec((1, rows, LANES), lambda c: (c, 0, 0)),
            pl.BlockSpec((1, PAD, LANES), lambda c: (c, 0, 0)),
            pl.BlockSpec((1,) + taps.shape[1:], lambda c: (c, 0, 0)),
            flat,
            flat,
        ],
        out_specs=[flat, flat],
        out_shape=[jax.ShapeDtypeStruct((rows, width), jnp.bfloat16)] * 2,
        scratch_shapes=[pltpu.VMEM((PAD + rows, LANES), jnp.float32)],
        cost_estimate=pl.CostEstimate(
            flops=rows * width * 75, bytes_accessed=rows * width * 12, transcendentals=0
        ),
        name="gated_back",
    )(grad_conv, after, taps, values_in, gates_in)


def chip_shift(value, chips, cores, steps):
    pairs = [
        (chip * cores + core, (chip + steps) % chips * cores + core)
        for chip in range(chips)
        for core in range(cores)
    ]
    return lax.ppermute(value, "dp", pairs)


def core_swap(value, chips, cores):
    return lax.ppermute(value, "dp", [(i, i ^ 1) for i in range(chips * cores)])


def bit_swap(value, axis, bit):
    count = lax.axis_size(axis)
    return lax.ppermute(value, axis, [(i, i ^ (1 << bit)) for i in range(count)])


def passed_along(value, axis, steps):
    count = lax.axis_size(axis)
    initial, last = (max(0, -steps), min(count, count - steps))
    return lax.ppermute(value, axis, [(source, source + steps) for source in range(initial, last)])


def gathered(value, axis):
    count = lax.axis_size(axis)
    bits = count.bit_length() - 1
    me = lax.axis_index(axis)
    whole = value[None]
    for bit in range(bits):
        other = bit_swap(whole, axis, bit)
        mine_first = ((me >> bit) & 1) == 0
        whole = jnp.where(
            mine_first,
            jnp.concatenate([whole, other], axis=0),
            jnp.concatenate([other, whole], axis=0),
        )
    return whole


def gated_forward(values_in, gates_in):
    return (values_in.astype(jnp.float32) * jax.nn.sigmoid(gates_in.astype(jnp.float32))).astype(
        jnp.bfloat16
    )


def scattered_sum(parts, axis):
    count = lax.axis_size(axis)
    bits = count.bit_length() - 1
    me = lax.axis_index(axis)
    for bit in range(bits):
        mine = (me >> bit) & 1
        pairs = parts.reshape((parts.shape[0] // 2, 2) + parts.shape[1:])
        keep = lax.dynamic_index_in_dim(pairs, mine, axis=1, keepdims=False)
        send = lax.dynamic_index_in_dim(pairs, 1 - mine, axis=1, keepdims=False)
        parts = keep + bit_swap(send.astype(jnp.bfloat16), axis, bit).astype(jnp.float32)
    return parts[0]


def shards(out_cotangent, value_pre, gate_pre, out_weight, conv_kernel, norm_gain):
    cotangent = out_cotangent[0]
    values_in = value_pre[0]
    gates_in = gate_pre[0]
    row_count, width = cotangent.shape
    taps_count = conv_kernel.shape[0]
    sp_count, dp_count = lax.axis_size("sp"), lax.axis_size("dp")
    cores = CORES if dp_count % CORES == 0 else 1
    chips = dp_count // cores
    place = lax.axis_index("dp")
    chip, core = place // cores, place % cores

    small = gathered(jnp.concatenate([conv_kernel, norm_gain[None]], axis=0), "sp")
    front = passed_along(
        gated_forward(values_in[row_count - PAD :], gates_in[row_count - PAD :]), "sp", 1
    )
    cots = [cotangent] + [chip_shift(cotangent, chips, cores, k) for k in range(1, chips)]
    weight_other = core_swap(out_weight, chips, cores) if cores > 1 else None

    def times_weights(cot):
        dims = (((1,), (1,)), ((), ()))
        mine = lax.dot_general(cot, out_weight, dims, preferred_element_type=jnp.float32)
        mine = mine.astype(jnp.bfloat16)
        if cores == 1:
            return mine
        other = lax.dot_general(cot, weight_other, dims, preferred_element_type=jnp.float32)
        other = other.astype(jnp.bfloat16)
        return jnp.where(
            core == 0,
            jnp.concatenate([mine, other], axis=1),
            jnp.concatenate([other, mine], axis=1),
        )

    taps = small.astype(jnp.float32)
    taps = taps.reshape(width // LANES if taps.shape[2] == LANES else sp_count, taps_count + 1, -1)
    if taps.shape[2] != LANES:
        taps = taps.reshape(sp_count, taps_count + 1, -1, LANES).transpose(0, 2, 1, 3)
        taps = taps.reshape(-1, taps_count + 1, LANES)
    activation, centred, gated, inv = forward(values_in, gates_in, front, taps, taps_count)

    grad_act = jnp.zeros((row_count, width), jnp.bfloat16)
    for k in range(chips):
        piece = times_weights(cots[k])
        if k:
            piece = chip_shift(piece, chips, cores, -k)
        grad_act = lax.dynamic_update_slice(
            grad_act, piece, (0, (chip + k) % chips * piece.shape[1])
        )

    rows_out = width // (sp_count * dp_count)
    act_parts = activation.reshape(row_count, sp_count, chips, cores * rows_out)

    def for_chip(k):
        part = lax.dynamic_index_in_dim(act_parts, (chip + k) % chips, axis=2, keepdims=False)
        return part.reshape(row_count, -1)

    acts = [for_chip(0)] + [
        chip_shift(for_chip(k), chips, cores, k) for k in range(1, chips)
    ]
    weight_part = sum(
        lax.dot_general(act, cot, (((0,), (0,)), ((), ())), preferred_element_type=jnp.float32)
        for act, cot in zip(acts, cots)
    )
    weight_part = weight_part.reshape(sp_count, cores, rows_out, width)
    if cores > 1:
        keep = lax.dynamic_index_in_dim(weight_part, core, axis=1, keepdims=False)
        send = lax.dynamic_index_in_dim(weight_part, 1 - core, axis=1, keepdims=False)
        send = core_swap(send.astype(jnp.bfloat16), chips, cores)
        weight_part = keep + send.astype(jnp.float32)
    else:
        weight_part = weight_part[:, 0]
    weight_sum = scattered_sum(weight_part, "sp")

    grad_conv, gain_part = normed_back(grad_act, centred, inv, taps, taps_count)
    after = passed_along(grad_conv[:, :PAD], "sp", -1)
    small_part = taps_back(grad_conv, gated, front, gain_part, taps_count)
    small_part = lax.all_to_all(small_part, "sp", 1, 0, tiled=True)
    small_part = jnp.sum(small_part.reshape(sp_count, taps_count + 1, -1), axis=0)
    small_sum = jnp.sum(lax.all_gather(small_part, "dp"), axis=0)
    grad_values, grad_gates = gated_back(grad_conv, after, taps, values_in, gates_in, taps_count)

    factor = float(sp_count * dp_count * row_count) ** (-0.5)
    return (
        grad_values[None],
        grad_gates[None],
        weight_sum * factor,
        small_sum[:taps_count] * factor,
        small_sum[taps_count] * factor,
    )


def solution(mesh):
    placed = (
        P("dp", "sp", None),
        P("dp", "sp", None),
        P("dp", "sp", None),
        P("dp", None),
        P(None, "sp"),
        P("sp"),
    )
    return jax.shard_map(
        shards,
        mesh=mesh,
        in_specs=placed,
        out_specs=(
            P("dp", "sp", None),
            P("dp", "sp", None),
            P(("sp", "dp"), None),
            P(None, "sp"),
            P("sp"),
        ),
        check_vma=False,
    )
```

```python
import functools

import jax
import jax.numpy as jnp
from jax import lax
from jax.experimental import pallas as pl
from jax.experimental.pallas import tpu as pltpu
from jax.sharding import PartitionSpec as P

epsilon = 1e-05
CORES = 2
LANES = 128
PAD = 32
BLOCK = 64
WHOLE = pl.BlockSpec(memory_space=pltpu.VMEM)


def sigmoid(value):
    return 1.0 / (1.0 + jnp.exp(-value))


def column(c):
    return pl.ds(pl.multiple_of(c * LANES, LANES), LANES)


def kernel_call(body, operands, outs, scratch, flops):
    moved = sum(a.size * a.dtype.itemsize for a in operands)
    moved += sum(o.size * o.dtype.itemsize for o in outs)
    return pl.pallas_call(
        body,
        in_specs=[WHOLE] * len(operands),
        out_specs=[WHOLE] * len(outs),
        out_shape=outs,
        scratch_shapes=scratch,
        compiler_params=pltpu.CompilerParams(vmem_limit_bytes=24 * 1024 * 1024),
        cost_estimate=pl.CostEstimate(flops=flops, bytes_accessed=moved, transcendentals=0),
    )(*operands)


def forward_body(taps_count, pieces, value, gate, front, taps, act, centred, gated, inv, held, total, mean):
    rows, width = value.shape
    columns = width // LANES
    blocks = [slice(b, b + BLOCK) for b in range(0, rows, BLOCK)]
    total[...] = jnp.zeros(total.shape, jnp.float32)

    def convolve(c, carry):
        lanes = column(c)
        held[:PAD, :] = front[:, lanes].astype(jnp.float32)
        for b in blocks:
            product = value[b, lanes].astype(jnp.float32) * sigmoid(gate[b, lanes].astype(jnp.float32))
            product = product.astype(jnp.bfloat16)
            gated[b, lanes] = product
            held[PAD + b.start : PAD + b.stop, :] = product.astype(jnp.float32)
        for b in blocks:
            result = jnp.zeros((BLOCK, LANES), jnp.float32)
            for k in range(taps_count):
                begin = PAD + b.start - k
                result = result + taps[c, k : k + 1, :] * held[begin : begin + BLOCK, :]
            centred[c, b, :] = result
            total[b, :] += result
        return carry

    lax.fori_loop(0, columns, convolve, 0)
    for b in blocks:
        centre = jnp.sum(total[b, :], axis=1, keepdims=True) * (1.0 / width)
        mean[b, :] = jnp.broadcast_to(centre, (BLOCK, LANES))
        total[b, :] = jnp.zeros((BLOCK, LANES), jnp.float32)

    def squares(c, carry):
        for b in blocks:
            off = centred[c, b, :] - mean[b, :]
            centred[c, b, :] = off
            total[b, :] += off * off
        return carry

    lax.fori_loop(0, columns, squares, 0)
    for b in blocks:
        variance = jnp.sum(total[b, :], axis=1, keepdims=True) * (1.0 / width)
        inv[b, :] = jnp.broadcast_to(lax.rsqrt(variance + epsilon), (BLOCK, LANES))

    def activate(c, b):
        value_c = centred[c, b, :] * inv[b, :]
        centred[c, b, :] = value_c
        normed = value_c * taps[c, taps_count : taps_count + 1, :]
        return normed * sigmoid(normed)

    if pieces is None:

        def normalize(c, carry):
            for b in blocks:
                act[b, column(c)] = activate(c, b).astype(jnp.bfloat16)
            return carry

        lax.fori_loop(0, columns, normalize, 0)
    else:
        chips = pieces
        half = LANES // 2

        def normalize(j, carry):
            for chip in range(chips):
                for b in blocks:
                    one = activate(2 * j * chips + chip, b)
                    two = activate((2 * j + 1) * chips + chip, b)
                    act[chip, 0, b, column(j)] = jnp.concatenate(
                        [one[:, :half], two[:, :half]], axis=1
                    ).astype(jnp.bfloat16)
                    act[chip, 1, b, column(j)] = jnp.concatenate(
                        [one[:, half:], two[:, half:]], axis=1
                    ).astype(jnp.bfloat16)
            return carry

        lax.fori_loop(0, columns // (2 * chips), normalize, 0)


def forward(values_in, gates_in, front, taps, taps_count, pieces):
    rows, width = values_in.shape
    columns = width // LANES
    shape = (rows, width) if pieces is None else (pieces, 2, rows, width // (2 * pieces))
    return kernel_call(
        functools.partial(forward_body, taps_count, pieces),
        (values_in, gates_in, front, taps),
        [
            jax.ShapeDtypeStruct(shape, jnp.bfloat16),
            jax.ShapeDtypeStruct((columns, rows, LANES), jnp.float32),
            jax.ShapeDtypeStruct((rows, width), jnp.bfloat16),
            jax.ShapeDtypeStruct((rows, LANES), jnp.float32),
        ],
        [
            pltpu.VMEM((PAD + rows, LANES), jnp.float32),
            pltpu.VMEM((rows, LANES), jnp.float32),
            pltpu.VMEM((rows, LANES), jnp.float32),
        ],
        rows * width * 100,
    )


def normed_back_body(taps_count, grad_act, centred, inv, taps, grad_conv, gain_part, first, second):
    rows, width = grad_act.shape
    columns = width // LANES
    blocks = [slice(b, b + BLOCK) for b in range(0, rows, BLOCK)]
    first[...] = jnp.zeros(first.shape, jnp.float32)
    second[...] = jnp.zeros(second.shape, jnp.float32)

    def products(c, carry):
        lanes = column(c)
        gain = taps[c, taps_count : taps_count + 1, :]
        part = jnp.zeros((8, LANES), jnp.float32)
        for b in blocks:
            centred_c = centred[c, b, :]
            normed = centred_c * gain
            sig = sigmoid(normed)
            grad_normed = grad_act[b, lanes].astype(jnp.float32) * (
                sig * (1.0 + normed * (1.0 - sig))
            )
            scaled = grad_normed * centred_c
            part = part + jnp.sum(scaled.reshape(BLOCK // 8, 8, LANES), axis=0)
            grad_centred = grad_normed * gain
            grad_conv[c, b, :] = grad_centred
            first[b, :] += grad_centred
            second[b, :] += scaled * gain
        gain_part[:, lanes] = part
        return carry

    lax.fori_loop(0, columns, products, 0)
    for b in blocks:
        mean = jnp.sum(first[b, :], axis=1, keepdims=True) * (1.0 / width)
        first[b, :] = jnp.broadcast_to(mean, (BLOCK, LANES))
        mean = jnp.sum(second[b, :], axis=1, keepdims=True) * (1.0 / width)
        second[b, :] = jnp.broadcast_to(mean, (BLOCK, LANES))

    def finish(c, carry):
        for b in blocks:
            grad_conv[c, b, :] = (
                grad_conv[c, b, :] - first[b, :] - centred[c, b, :] * second[b, :]
            ) * inv[b, :]
        return carry

    lax.fori_loop(0, columns, finish, 0)


def normed_back(grad_act, centred, inv, taps, taps_count):
    rows, width = grad_act.shape
    return kernel_call(
        functools.partial(normed_back_body, taps_count),
        (grad_act, centred, inv, taps),
        [
            jax.ShapeDtypeStruct((width // LANES, rows, LANES), jnp.float32),
            jax.ShapeDtypeStruct((8, width), jnp.float32),
        ],
        [pltpu.VMEM((rows, LANES), jnp.float32), pltpu.VMEM((rows, LANES), jnp.float32)],
        rows * width * 40,
    )


def taps_back_body(taps_count, grad_conv, gated, front, gain_part, out, held):
    rows, width = gated.shape

    def one(c, carry):
        lanes = column(c)
        held[:PAD, :] = front[:, lanes].astype(jnp.float32)
        held[PAD:, :] = gated[:, lanes].astype(jnp.float32)
        sums = [jnp.zeros((8, LANES), jnp.float32) for _ in range(taps_count)]
        for j in range(0, rows, 8):
            grad = grad_conv[c, j : j + 8, :]
            for k in range(taps_count):
                begin = j + PAD - k
                sums[k] = sums[k] + grad * held[begin : begin + 8, :]
        for k in range(taps_count):
            out[k : k + 1, lanes] = jnp.sum(sums[k], axis=0, keepdims=True)
        out[taps_count : taps_count + 1, lanes] = jnp.sum(gain_part[:, lanes], axis=0, keepdims=True)
        return carry

    lax.fori_loop(0, width // LANES, one, 0)


def taps_back(grad_conv, gated, front, gain_part, taps_count):
    rows, width = gated.shape
    return kernel_call(
        functools.partial(taps_back_body, taps_count),
        (grad_conv, gated, front, gain_part),
        [jax.ShapeDtypeStruct((taps_count + 1, width), jnp.float32)],
        [pltpu.VMEM((PAD + rows, LANES), jnp.float32)],
        rows * width * 62,
    )[0]


def gated_back_body(taps_count, grad_conv, after, taps, value, gate, grad_value, grad_gate, held):
    rows, width = value.shape

    def one(c, carry):
        lanes = column(c)
        held[:rows, :] = grad_conv[c]
        held[rows:, :] = after[c]
        for begin in range(0, rows, BLOCK):
            result = jnp.zeros((BLOCK, LANES), jnp.float32)
            for k in range(taps_count):
                result = result + taps[c, k : k + 1, :] * held[begin + k : begin + k + BLOCK, :]
            result = result.astype(jnp.bfloat16).astype(jnp.float32)
            b = slice(begin, begin + BLOCK)
            sig = sigmoid(gate[b, lanes].astype(jnp.float32))
            grad_sig = result * sig
            grad_value[b, lanes] = grad_sig.astype(jnp.bfloat16)
            grad_gate[b, lanes] = (
                grad_sig * value[b, lanes].astype(jnp.float32) * (1.0 - sig)
            ).astype(jnp.bfloat16)
        return carry

    lax.fori_loop(0, width // LANES, one, 0)


def gated_back(grad_conv, after, taps, values_in, gates_in, taps_count):
    rows, width = values_in.shape
    return kernel_call(
        functools.partial(gated_back_body, taps_count),
        (grad_conv, after, taps, values_in, gates_in),
        [jax.ShapeDtypeStruct((rows, width), jnp.bfloat16)] * 2,
        [pltpu.VMEM((PAD + rows, LANES), jnp.float32)],
        rows * width * 75,
    )


def chip_shift(value, chips, cores, steps):
    pairs = [
        (chip * cores + core, (chip + steps) % chips * cores + core)
        for chip in range(chips)
        for core in range(cores)
    ]
    return lax.ppermute(value, "dp", pairs)


def core_swap(value, chips, cores):
    return lax.ppermute(value, "dp", [(i, i ^ 1) for i in range(chips * cores)])


def bit_swap(value, axis, bit):
    count = lax.axis_size(axis)
    return lax.ppermute(value, axis, [(i, i ^ (1 << bit)) for i in range(count)])


def passed_along(value, axis, steps):
    count = lax.axis_size(axis)
    initial, last = (max(0, -steps), min(count, count - steps))
    return lax.ppermute(value, axis, [(source, source + steps) for source in range(initial, last)])


def gathered(value, axis):
    count = lax.axis_size(axis)
    bits = count.bit_length() - 1
    me = lax.axis_index(axis)
    whole = value[None]
    for bit in range(bits):
        other = bit_swap(whole, axis, bit)
        mine_first = ((me >> bit) & 1) == 0
        whole = jnp.where(
            mine_first,
            jnp.concatenate([whole, other], axis=0),
            jnp.concatenate([other, whole], axis=0),
        )
    return whole


def gated_forward(values_in, gates_in):
    return (values_in.astype(jnp.float32) * jax.nn.sigmoid(gates_in.astype(jnp.float32))).astype(
        jnp.bfloat16
    )


def scattered_sum(parts, axis):
    count, _, width = parts.shape
    bits = count.bit_length() - 1
    me = lax.axis_index(axis)
    orders = [list(range(bits)), list(range(bits // 2, bits)) + list(range(bits // 2))]
    cut = width // 2
    flows = [parts[:, :, :cut], parts[:, :, cut:]]
    flows = [flow.reshape((2,) * bits + flow.shape[1:]) for flow in flows]
    left = [list(range(bits)), list(range(bits))]
    for step in range(bits):
        for f in range(2):
            bit = orders[f][step]
            dim = len(left[f]) - 1 - left[f].index(bit)
            left[f].remove(bit)
            mine = (me >> bit) & 1
            keep = lax.dynamic_index_in_dim(flows[f], mine, axis=dim, keepdims=False)
            send = lax.dynamic_index_in_dim(flows[f], 1 - mine, axis=dim, keepdims=False)
            came = bit_swap(send.astype(jnp.bfloat16), axis, bit)
            flows[f] = keep + came.astype(jnp.float32)
    return jnp.concatenate(flows, axis=1)


def shards(out_cotangent, value_pre, gate_pre, out_weight, conv_kernel, norm_gain):
    return step(
        out_cotangent[0], value_pre[0], gate_pre[0], out_weight, conv_kernel, norm_gain
    )


def step(cotangent, values_in, gates_in, out_weight, conv_kernel, norm_gain):
    row_count, width = cotangent.shape
    taps_count = conv_kernel.shape[0]
    sp_count, dp_count = lax.axis_size("sp"), lax.axis_size("dp")
    cores = CORES
    chips = dp_count // cores
    place = lax.axis_index("dp")
    chip, core = place // cores, place % cores
    pieces = chips if width // (sp_count * chips) == LANES else None

    cots = [cotangent]
    for k in range(1, chips):
        cots.append(chip_shift(cotangent, chips, cores, k))
    small = gathered(jnp.concatenate([conv_kernel, norm_gain[None]], axis=0), "sp")
    front = passed_along(
        gated_forward(values_in[row_count - PAD :], gates_in[row_count - PAD :]), "sp", 1
    )
    weight_other = core_swap(out_weight, chips, cores)

    def times_weights(cot):
        dims = (((1,), (1,)), ((), ()))
        mine = lax.dot_general(cot, out_weight, dims, preferred_element_type=jnp.float32)
        other = lax.dot_general(cot, weight_other, dims, preferred_element_type=jnp.float32)
        mine, other = mine.astype(jnp.bfloat16), other.astype(jnp.bfloat16)
        return jnp.where(
            core == 0,
            jnp.concatenate([mine, other], axis=1),
            jnp.concatenate([other, mine], axis=1),
        )

    taps = small.astype(jnp.float32)
    if taps.shape[2] > LANES:
        taps = taps.reshape(sp_count, taps_count + 1, -1, LANES).transpose(0, 2, 1, 3)
    taps = taps.reshape(-1, taps_count + 1, LANES)
    activation, centred, gated, inv = forward(values_in, gates_in, front, taps, taps_count, pieces)

    rows_out = width // (sp_count * dp_count)
    if pieces is None:
        activation = activation.reshape(row_count, sp_count, chips, cores, rows_out)
        activation = activation.transpose(2, 3, 0, 1, 4).reshape(chips, cores, row_count, -1)
    act_mine = lax.dynamic_index_in_dim(activation, core, axis=1, keepdims=False)
    act_send = lax.dynamic_index_in_dim(activation, 1 - core, axis=1, keepdims=False)
    act_other = core_swap(act_send, chips, cores)
    act_pair = jnp.concatenate([act_mine, act_other], axis=1)
    acts = [lax.dynamic_index_in_dim(act_pair, chip, axis=0, keepdims=False)]
    for k in range(1, chips):
        part = lax.dynamic_index_in_dim(act_pair, (chip + k) % chips, axis=0, keepdims=False)
        acts.append(chip_shift(part, chips, cores, k))

    grad_act = jnp.zeros((row_count, width), jnp.bfloat16)
    for k in list(range(1, chips)) + [0]:
        piece = times_weights(cots[k])
        if k:
            piece = chip_shift(piece, chips, cores, -k)
        grad_act = lax.dynamic_update_slice(
            grad_act, piece, (0, (chip + k) % chips * piece.shape[1])
        )

    weight_part = 0.0
    for act, cot in zip(acts, cots):
        other = core_swap(cot, chips, cores)
        for left, right in ((act[:row_count], cot), (act[row_count:], other)):
            weight_part = weight_part + lax.dot_general(
                left, right, (((0,), (0,)), ((), ())), preferred_element_type=jnp.float32
            )
    weight_sum = scattered_sum(weight_part.reshape(sp_count, rows_out, width), "sp")

    grad_conv, gain_part = normed_back(grad_act, centred, inv, taps, taps_count)
    after = passed_along(grad_conv[:, :PAD], "sp", -1)
    small_part = taps_back(grad_conv, gated, front, gain_part, taps_count)
    small_part = lax.all_to_all(small_part, "sp", 1, 0, tiled=True)
    small_part = jnp.sum(small_part.reshape(sp_count, taps_count + 1, -1), axis=0)
    small_sum = jnp.sum(lax.all_gather(small_part, "dp"), axis=0)
    grad_values, grad_gates = gated_back(grad_conv, after, taps, values_in, gates_in, taps_count)

    factor = float(sp_count * dp_count * row_count) ** (-0.5)
    return (
        grad_values[None],
        grad_gates[None],
        weight_sum * factor,
        small_sum[:taps_count] * factor,
        small_sum[taps_count] * factor,
    )


def solution(mesh):
    placed = (
        P("dp", "sp", None),
        P("dp", "sp", None),
        P("dp", "sp", None),
        P("dp", None),
        P(None, "sp"),
        P("sp"),
    )
    return jax.shard_map(
        shards,
        mesh=mesh,
        in_specs=placed,
        out_specs=(
            P("dp", "sp", None),
            P("dp", "sp", None),
            P(("sp", "dp"), None),
            P(None, "sp"),
            P("sp"),
        ),
        check_vma=False,
    )
```
